512 devices in a mesh: sp: 32 (over z, core), tp: 16 (over y, x).
Axes of the slice: x: 4, y: 4, z: 16, core: 2. Of those that a mesh axis runs over, the one named last changes fastest.
Arguments:
- stream: bfloat16 [4096, 2048], P('sp'), may hold values from -6 to 6
- query_small: bfloat16 [4096, 1024], P('sp', 'tp'), may hold values from -6 to 6
- key_small: bfloat16 [4096, 1024], P('sp', 'tp'), may hold values from -6 to 6
- value_small: bfloat16 [4096, 1024], P('sp', 'tp'), may hold values from -6 to 6
- query_large: bfloat16 [4096, 2048], P('sp', 'tp'), may hold values from -6 to 6
- key_large: bfloat16 [4096, 2048], P('sp', 'tp'), may hold values from -6 to 6
- value_large: bfloat16 [4096, 2048], P('sp', 'tp'), may hold values from -6 to 6
- key_bias: bfloat16 [4096, 2, 16], P('sp', None, 'tp'), may hold values from -16 to 1
- out_small: bfloat16 [1024, 2048], P('tp'), may hold values from -0.75 to 0.75
- out_large: bfloat16 [2048, 2048], P('tp'), may hold values from -0.75 to 0.75
- gain_one: float32 [2048], replicated, may hold values from 0.1 to 1.9
- shift_one: float32 [2048], replicated, may hold values from -1.5 to 1.5
- gain_two: float32 [2048], replicated, may hold values from 0.1 to 1.9
- shift_two: float32 [2048], replicated, may hold values from -1.5 to 1.5
- expert_pick: int32 [4096, 2], P('sp'), may hold values from 0 to 31, as said below
- route_weight: float32 [4096, 2], P('sp'), may hold values from 0.2 to 1
- w_gate: bfloat16 [32, 2048, 4096], P('sp', None, 'tp'), may hold values from -0.125 to 0.125
- w_up: bfloat16 [32, 2048, 4096], P('sp', None, 'tp'), may hold values from -0.125 to 0.125
- w_down: bfloat16 [32, 4096, 2048], P('sp', 'tp'), may hold values from -0.09375 to 0.09375
Outputs:
- result: bfloat16 [4096, 2048], P(('sp', 'tp'))
The draws below stay inside these ranges and needn't reach their ends.
Inputs may be any that keep to these rules, and one draw needn't show every extreme that they name: In each aligned block of 128 positions (the positions of one index of sp), no expert is named more than 16 times, and in every block some expert is named exactly 16 times. The two experts of a position differ and lie in one group: equal values of expert_pick // 8.
All inputs are finite; a program needn't handle non-finite values.
Results may differ from the reference program's by a relative error of at most 0.017.
Values may be sent and summed in bfloat16 or wider, within the bound.
No kernel may reach another device: no remote copies, remote signals or barrier semaphores. Data moves between devices by JAX's collectives and lax.ppermute only.
A program may use at most 64 MiB of HBM per device.

```python
import jax
import jax.numpy as jnp
from jax import lax

D = 2048
HEADS_PER_GROUP = 16
HEAD_SMALL = 64
HEAD_LARGE = 128
FF_E = 4096
GROUPS = 4
TOK_DEV = 128
SEQUENCE_LENGTH = 4096
EXPERTS = 32
PER_GROUP = 8
CAP = 16
N_TP = 16


def draw_key_bias(key, part):
    key_matrix = jax.random.split(key, 7)
    head_shape = (2, HEADS_PER_GROUP)
    fast_share = 0.5
    slow_low = 1.0
    slow_high = 2.0
    fast_heads = jax.random.uniform(key_matrix[0], head_shape) < fast_share
    slow_rate = jax.random.uniform(key_matrix[1], head_shape, minval=slow_low, maxval=slow_high) / SEQUENCE_LENGTH
    fast_rate = 1.0 / jax.random.uniform(key_matrix[2], head_shape, minval=30.0, maxval=100.0)
    rate = jnp.where(fast_heads, fast_rate, slow_rate)
    block_factor = jnp.exp(jax.random.uniform(key_matrix[3], (SEQUENCE_LENGTH // TOK_DEV, 2, HEADS_PER_GROUP), minval=-0.7, maxval=0.7))
    block_factor = jnp.repeat(block_factor, TOK_DEV, axis=0)
    baseline_logit = jnp.log(rate[None] * block_factor) - 0.5
    spike_mask = jax.random.uniform(key_matrix[4], (SEQUENCE_LENGTH, 2, HEADS_PER_GROUP)) < 2.0 / SEQUENCE_LENGTH
    spike_level = jax.random.uniform(key_matrix[5], (SEQUENCE_LENGTH, 2, HEADS_PER_GROUP), minval=0.2, maxval=0.5)
    spike_logit = jnp.log(spike_level / (1.0 - spike_level))
    perturbation_term = 0.3 * jax.random.normal(key_matrix[6], (SEQUENCE_LENGTH, 2, HEADS_PER_GROUP))
    sampled_values = jnp.where(spike_mask, spike_logit, baseline_logit + perturbation_term)
    return sampled_values.astype(jnp.float32).astype(jnp.bfloat16)


def value_field(key, columns):
    key_matrix = jax.random.split(key, 2)
    sampled_values = jnp.clip(jax.random.normal(key_matrix[1], (SEQUENCE_LENGTH, columns)), -6.0, 6.0)
    return sampled_values.astype(jnp.float32).astype(jnp.bfloat16)


def draw_value_small(key, part):
    return value_field(jax.random.fold_in(key, 101), HEADS_PER_GROUP * HEAD_SMALL)


def draw_value_large(key, part):
    return value_field(jax.random.fold_in(key, 202), HEADS_PER_GROUP * HEAD_LARGE)


def group_cycle(sub_key):
    return jax.random.permutation(sub_key, PER_GROUP).astype(jnp.int32)


def pick_block(key):
    key_matrix = jax.random.split(key, 4)
    order = jnp.argsort(jax.random.permutation(key_matrix[0], TOK_DEV)).astype(jnp.int32)
    group_cap = PER_GROUP * CAP // 2
    group_order = jax.random.permutation(key_matrix[1], GROUPS).astype(jnp.int32)
    cut_pair = jax.random.randint(key_matrix[2], (2,), group_cap, TOK_DEV + 1).astype(jnp.int32)
    cut_low = jnp.min(cut_pair)
    cut_high = jnp.max(cut_pair)
    bucket = (order >= group_cap).astype(jnp.int32) + (order >= cut_low).astype(jnp.int32) + (order >= cut_high).astype(jnp.int32)
    offsets = jnp.stack([jnp.int32(0), jnp.int32(group_cap), cut_low, cut_high])
    in_group = order - offsets[bucket]
    group_id = group_order[bucket]
    cycles = jax.vmap(group_cycle)(jax.random.split(key_matrix[3], GROUPS))
    first_pick = cycles[group_id, 2 * in_group % PER_GROUP]
    second_pick = cycles[group_id, (2 * in_group + 1) % PER_GROUP]
    return jnp.stack([group_id * PER_GROUP + first_pick, group_id * PER_GROUP + second_pick], axis=-1).astype(jnp.int32)


def draw_expert_pick(key, part):
    return jax.vmap(pick_block)(jax.random.split(key, SEQUENCE_LENGTH // TOK_DEV)).reshape(SEQUENCE_LENGTH, 2)


def level_of(key, extent, cuts, smallest, high):
    factor_of, own = 1.0, jax.random.fold_in(key, 6)
    for position, parts in cuts:
        heights = jnp.exp(jax.random.uniform(jax.random.fold_in(own, position), (parts,), jnp.float32, smallest / len(cuts), high / len(cuts)))
        factor_of = factor_of * jnp.repeat(heights, extent[position] // parts).reshape([-1 if axis == position else 1 for axis in range(len(extent))])
    return factor_of


def bell_draw(own_key, dims, scale, bound, cuts=(), held_as=jnp.bfloat16):
    values = scale * jax.random.normal(own_key, dims, jnp.float32)
    if cuts:
        values = values * level_of(own_key, dims, cuts, -0.22, 0.18)
    return jnp.clip(values, -bound, bound).astype(held_as)


def setup_inputs(seed: int = 0) -> dict:
    key_list = jax.random.split(jax.random.key(seed), 20)
    stream = bell_draw(key_list[0], (SEQUENCE_LENGTH, D), 1.0, 6.0, ((0, 32),))
    query_small = bell_draw(key_list[1], (SEQUENCE_LENGTH, HEADS_PER_GROUP * HEAD_SMALL), 1.0, 6.0, ((0, 32), (1, 16)))
    key_small = bell_draw(key_list[2], (SEQUENCE_LENGTH, HEADS_PER_GROUP * HEAD_SMALL), 1.0, 6.0, ((0, 32), (1, 16)))
    value_small = draw_value_small(jax.random.fold_in(key_list[19], 71), 0)
    query_large = bell_draw(key_list[4], (SEQUENCE_LENGTH, HEADS_PER_GROUP * HEAD_LARGE), 1.0, 6.0, ((0, 32), (1, 16)))
    key_large = bell_draw(key_list[5], (SEQUENCE_LENGTH, HEADS_PER_GROUP * HEAD_LARGE), 1.0, 6.0, ((0, 32), (1, 16)))
    value_large = draw_value_large(jax.random.fold_in(key_list[19], 71), 0)
    key_bias = draw_key_bias(jax.random.fold_in(key_list[19], 71), 0)
    out_small = bell_draw(key_list[8], (HEADS_PER_GROUP * HEAD_SMALL, D), (HEADS_PER_GROUP * (HEAD_SMALL + HEAD_LARGE) // 48) ** -0.5, 0.75, ((0, 16),))
    out_large = bell_draw(key_list[9], (HEADS_PER_GROUP * HEAD_LARGE, D), (HEADS_PER_GROUP * (HEAD_SMALL + HEAD_LARGE) // 48) ** -0.5, 0.75, ((0, 16),))
    gain_one = jnp.clip(1.0 + 0.18 * jax.random.normal(key_list[10], (D,), jnp.float32), 0.1, 1.9)
    shift_one = bell_draw(key_list[11], (D,), 0.3, 1.5, (), jnp.float32)
    gain_two = jnp.clip(1.0 + 0.18 * jax.random.normal(key_list[12], (D,), jnp.float32), 0.1, 1.9)
    shift_two = bell_draw(key_list[13], (D,), 0.3, 1.5, (), jnp.float32)
    expert_pick = draw_expert_pick(jax.random.fold_in(key_list[19], 71), 0)
    route_weight = jnp.clip(0.2 + 0.8 * jax.random.uniform(key_list[15], (SEQUENCE_LENGTH, 2), jnp.float32) ** level_of(key_list[15], (SEQUENCE_LENGTH, 2), ((0, 32),), -0.2, 0.2), 0.2, 1.0)
    w_gate = bell_draw(key_list[16], (EXPERTS, D, FF_E), D ** -0.5, 0.125, ((0, 32), (2, 16)))
    w_up = bell_draw(key_list[17], (EXPERTS, D, FF_E), D ** -0.5, 0.125, ((0, 32), (2, 16)))
    w_down = bell_draw(key_list[18], (EXPERTS, FF_E, D), FF_E ** -0.5, 0.09375, ((0, 32), (1, 16)))
    return dict(stream=stream, query_small=query_small, key_small=key_small, value_small=value_small, query_large=query_large, key_large=key_large, value_large=value_large, key_bias=key_bias, out_small=out_small, out_large=out_large, gain_one=gain_one, shift_one=shift_one, gain_two=gain_two, shift_two=shift_two, expert_pick=expert_pick, route_weight=route_weight, w_gate=w_gate, w_up=w_up, w_down=w_down)


ALPHA_RES = 2.0 ** 0.25
NORM_EPS = 1e-05

def layer_norm(inputs, gain_vec, shift_vec):
    average = lax.optimization_barrier(jnp.mean(inputs, axis=-1, keepdims=True))
    centred = inputs - average
    variance = lax.optimization_barrier(jnp.mean(centred * centred, axis=-1, keepdims=True))
    return centred * lax.rsqrt(variance + NORM_EPS) * gain_vec + shift_vec

def stick_head(queries, key_rows, value_rows, log_bias):
    score_scale = queries.shape[1] ** (-0.5)
    outputs = []
    for block in range(SEQUENCE_LENGTH // TOK_DEV):
        first_row = block * TOK_DEV
        last_row = first_row + TOK_DEV
        scores = jnp.dot(queries[first_row:last_row], key_rows[:last_row].T, preferred_element_type=jnp.float32)
        scores = scores * score_scale + log_bias[:last_row].astype(jnp.float32)[None, :]
        query_pos = first_row + jnp.arange(TOK_DEV)
        key_pos = jnp.arange(last_row)
        causal = key_pos[None, :] < query_pos[:, None]
        log_stay = jnp.where(causal, jax.nn.log_sigmoid(-scores), 0.0)
        later_sum = lax.cumsum(log_stay, axis=1, reverse=True) - log_stay
        stick = jnp.where(causal, jnp.exp(jax.nn.log_sigmoid(scores) + later_sum), 0.0)
        outputs.append(jnp.dot(stick.astype(jnp.bfloat16), value_rows[:last_row], preferred_element_type=jnp.float32))
    return jnp.concatenate(outputs, 0).astype(jnp.bfloat16)

def stick_group(queries, key_rows, value_rows, log_bias):
    head_size = queries.shape[1] // HEADS_PER_GROUP

    def split_heads(array):
        return array.reshape(SEQUENCE_LENGTH, HEADS_PER_GROUP, head_size).transpose(1, 0, 2)

    def one_head(packed):
        return stick_head(packed[0], packed[1], packed[2], packed[3])
    outputs = lax.map(one_head, (split_heads(queries), split_heads(key_rows), split_heads(value_rows), log_bias.T))
    return outputs.transpose(1, 0, 2).reshape(SEQUENCE_LENGTH, HEADS_PER_GROUP * head_size)

def reference(stream, query_small, key_small, value_small, query_large, key_large, value_large, key_bias, out_small, out_large, gain_one, shift_one, gain_two, shift_two, expert_pick, route_weight, w_gate, w_up, w_down):
    att_small = stick_group(query_small, key_small, value_small, key_bias[:, 0, :])
    att_large = stick_group(query_large, key_large, value_large, key_bias[:, 1, :])
    run_heads = HEADS_PER_GROUP // N_TP
    small_cols = run_heads * HEAD_SMALL
    large_cols = run_heads * HEAD_LARGE
    mixer_out = jnp.zeros((SEQUENCE_LENGTH, D), jnp.float32)
    for shard_index in range(N_TP):
        term = jnp.dot(att_small[:, shard_index * small_cols:(shard_index + 1) * small_cols], out_small[shard_index * small_cols:(shard_index + 1) * small_cols], preferred_element_type=jnp.float32)
        term = term + jnp.dot(att_large[:, shard_index * large_cols:(shard_index + 1) * large_cols], out_large[shard_index * large_cols:(shard_index + 1) * large_cols], preferred_element_type=jnp.float32)
        mixer_out = mixer_out + lax.optimization_barrier(term.astype(jnp.bfloat16)).astype(jnp.float32)
    normed = layer_norm(ALPHA_RES * stream.astype(jnp.float32) + mixer_out, gain_one, shift_one).astype(jnp.bfloat16)
    blocks = SEQUENCE_LENGTH // TOK_DEV
    picks = expert_pick.reshape(blocks, TOK_DEV * 2)
    one_hot = (picks[:, :, None] == jnp.arange(EXPERTS)[None, None, :]).astype(jnp.int32)
    slot_rank = lax.optimization_barrier(jnp.sum((jnp.cumsum(one_hot, axis=1) - one_hot) * one_hot, axis=2)).astype(jnp.int32)
    block_ids = jnp.broadcast_to(jnp.arange(blocks, dtype=jnp.int32)[:, None], picks.shape)
    token_of = (jnp.arange(TOK_DEV * 2, dtype=jnp.int32) // 2)[None, :] + block_ids * TOK_DEV
    slot_table = jnp.zeros((EXPERTS, blocks, CAP), jnp.int32).at[picks, block_ids, slot_rank].set(token_of)
    width = FF_E // N_TP

    def expert_rows(packed):
        table, gate_w, up_w, down_w = packed
        rows_in = normed[table.reshape(-1)]
        gate = jnp.dot(rows_in, gate_w, preferred_element_type=jnp.float32)
        upper = jnp.dot(rows_in, up_w, preferred_element_type=jnp.float32)
        hidden = (jax.nn.silu(gate) * upper).astype(jnp.bfloat16)
        running = jnp.zeros((rows_in.shape[0], D), jnp.float32)
        for shard_index in range(N_TP):
            term = jnp.dot(hidden[:, shard_index * width:(shard_index + 1) * width], down_w[shard_index * width:(shard_index + 1) * width], preferred_element_type=jnp.float32)
            running = running + lax.optimization_barrier(term.astype(jnp.bfloat16)).astype(jnp.float32)
        return running.astype(jnp.bfloat16)
    results = lax.map(expert_rows, (slot_table, w_gate, w_up, w_down)).reshape(EXPERTS, blocks, CAP, D)
    chosen = results[picks, block_ids, slot_rank].reshape(SEQUENCE_LENGTH, 2, D).astype(jnp.float32)
    expert_mix = chosen[:, 0] * route_weight[:, 0:1] + chosen[:, 1] * route_weight[:, 1:2]
    return layer_norm(ALPHA_RES * normed.astype(jnp.float32) + expert_mix, gain_two, shift_two).astype(jnp.bfloat16)
```

```python
import jax
import jax.numpy as jnp
from jax import lax
from jax.experimental import pallas as pl
from jax.experimental.pallas import tpu as pltpu
from jax.sharding import Mesh
from jax.sharding import PartitionSpec as P

SP = ("a", "b", "c")
TP = ("y", "x")
ALPHA_RES = 2.0**0.25
NORM_EPS = 1e-05
BF16 = jnp.bfloat16
F32 = jnp.float32


def call(body, out_shape, *args, scratch=(), name=None):
    return pl.pallas_call(
        body,
        out_shape=out_shape,
        scratch_shapes=list(scratch),
        compiler_params=pltpu.CompilerParams(vmem_limit_bytes=48 * 1024 * 1024),
        name=name,
    )(*args)


def contract(lhs, rhs, dims):
    return lax.dot_general(lhs, rhs, (dims, ((), ())), preferred_element_type=F32)


def pack_body(ks, vs, kl, vl, qs, ql, bias, kv_out, q_out):
    for i in range(kv_out.shape[0]):
        kv_out[i, 0:128, 0:64] = ks[...]
        kv_out[i, 0:128, 64:128] = vs[...]
        kv_out[i, 0:128, 128:256] = kl[...]
        kv_out[i, 0:128, 256:384] = vl[...]
        kv_out[i, 128:144, :] = bias[...]
    q_out[:, 0:64] = qs[...]
    q_out[:, 64:128] = jnp.zeros((128, 64), BF16)
    q_out[:, 128:256] = ql[...]


def gather_keys(own, other, kv, bias, c):
    for b in range(4):
        for core in range(2):
            block = jnp.where(c == core, own[b], other[b])
            row = (2 * b + core) * 128
            kv[pl.ds(row, 128), :] = block[0:128]
            bias[0:1, pl.ds(row, 128)] = block[128:144, 0:128].astype(F32)[0:1]
            bias[1:2, pl.ds(row, 128)] = block[128:144, 128:256].astype(F32)[0:1]


def stick_tile(q, k, v, bias, scale, later, carry, mask):
    acc, stay = carry
    s = contract(q, k, ((1,), (1,))) * scale + bias
    soft = jnp.log1p(jnp.exp(-jnp.abs(s)))
    log_take = jnp.minimum(s, 0.0) - soft
    log_stay = log_take - s
    if mask is not None:
        log_stay = jnp.where(mask, log_stay, 0.0)
    high = log_stay.astype(BF16)
    low = (log_stay - high.astype(F32)).astype(BF16)
    sums = contract(high, later, ((1,), (0,))) + contract(low, later, ((1,), (0,)))
    w = jnp.exp(log_take + sums + stay)
    if mask is not None:
        w = jnp.where(mask, w, 0.0)
    acc = acc + contract(w.astype(BF16), v, ((1,), (0,)))
    stay = stay + sums[:, 0:1] + log_stay[:, 0:1]
    return acc, stay


def stick_rows(q, kv, bias, row_pos):
    rows = q.shape[0]
    width = 256
    j = lax.broadcasted_iota(jnp.int32, (width, width), 0)
    i = lax.broadcasted_iota(jnp.int32, (width, width), 1)
    later = jnp.where(j > i, 1.0, 0.0).astype(BF16)
    carry = [
        (jnp.zeros((rows, 128), F32), jnp.zeros((rows, 1), F32)),
        (jnp.zeros((rows, 128), F32), jnp.zeros((rows, 1), F32)),
    ]
    for block in reversed(range(4)):
        at = block * width
        mask = None
        if row_pos is not None:
            r = lax.broadcasted_iota(jnp.int32, (rows, width), 0) + row_pos
            mask = lax.broadcasted_iota(jnp.int32, (rows, width), 1) + at < r
        keys = kv[at : at + width, :]
        carry[0] = stick_tile(
            q[:, 0:128], keys[:, 0:128], keys[:, 0:128],
            bias[0:1, at : at + width], 64.0**-0.5, later, carry[0], mask,
        )
        carry[1] = stick_tile(
            q[:, 128:256], keys[:, 128:256], keys[:, 256:384],
            bias[1:2, at : at + width], 128.0**-0.5, later, carry[1], mask,
        )
    return carry


def with_stay(carry):
    (acc_s, stay_s), (acc_l, stay_l) = carry
    lane = lax.broadcasted_iota(jnp.int32, acc_s.shape, 1)
    high_s = stay_s.astype(BF16).astype(F32)
    high_l = stay_l.astype(BF16).astype(F32)
    head = jnp.where(lane == 0, high_s, jnp.where(lane == 1, stay_s - high_s, 0.0))
    head = jnp.where(lane == 2, high_l, jnp.where(lane == 3, stay_l - high_l, head))
    return jnp.where(lane < 64, head, acc_s), acc_l


def far_body(place, q1, q2, q3, own, other, o1, o2, o3, kv, bias, q):
    a = place[0]
    for n, ref in enumerate((q1, q2, q3)):
        q[n * 128 : (n + 1) * 128, :] = ref[...]

    @pl.when(a < 3)
    def _():
        gather_keys(own, other, kv, bias, place[1])
        first, second = with_stay(stick_rows(q[...], kv, bias, None))
        for n, ref in enumerate((o1, o2, o3)):
            ref[:, 0:128] = first[n * 128 : (n + 1) * 128].astype(BF16)
            ref[:, 128:256] = second[n * 128 : (n + 1) * 128].astype(BF16)

    @pl.when(a == 3)
    def _():
        for ref in (o1, o2, o3):
            ref[...] = jnp.zeros((128, 256), BF16)


def near_body(place, q, own, other, o, kv, bias):
    gather_keys(own, other, kv, bias, place[1])
    row_pos = (place[2] * 2 + place[1]) * 128
    first, second = with_stay(stick_rows(q[...], kv, bias, row_pos))
    o[:, 0:128] = first
    o[:, 128:256] = second


def project_body(o0, o1, o2, o3, w_small, w_large, out):
    att_s = o0[:, 0:128]
    att_l = o0[:, 128:256]
    stay_s = att_s[:, 0:1] + att_s[:, 1:2]
    stay_l = att_s[:, 2:3] + att_s[:, 3:4]
    for ref in (o1, o2, o3):
        part = ref[:, 0:128].astype(F32)
        att_s = att_s + jnp.exp(stay_s) * part
        att_l = att_l + jnp.exp(stay_l) * ref[:, 128:256].astype(F32)
        stay_s = stay_s + part[:, 0:1] + part[:, 1:2]
        stay_l = stay_l + part[:, 2:3] + part[:, 3:4]
    att_s = att_s[:, 64:128].astype(BF16)
    att_l = att_l.astype(BF16)
    for n in range(8):
        cols = slice(n * 256, (n + 1) * 256)
        part = contract(att_s, w_small[:, cols], ((1,), (0,)))
        part = (part + contract(att_l, w_large[:, cols], ((1,), (0,)))).astype(BF16)
        out[2 * n] = part[:, 0:128]
        out[2 * n + 1] = part[:, 128:256]


def route_body(place, arrived, stream, picks, u_out, slot_out, out):
    total = ALPHA_RES * stream[...].astype(F32)
    mixed = arrived[0].astype(F32)
    for n in range(1, 16):
        mixed = mixed + arrived[n].astype(F32)
    u = (total + mixed).astype(BF16)
    u_out[...] = u
    expert = lax.broadcasted_iota(jnp.int32, (32, 128), 0)
    hot0 = jnp.where(expert == picks[0:1, :], 1.0, 0.0)
    hot1 = jnp.where(expert == picks[1:2, :], 1.0, 0.0)
    j = lax.broadcasted_iota(jnp.int32, (128, 128), 0)
    i = lax.broadcasted_iota(jnp.int32, (128, 128), 1)
    before = jnp.where(j < i, 1.0, 0.0).astype(BF16)
    count = contract((hot0 + hot1).astype(BF16), before, ((1,), (0,)))
    rank0 = jnp.sum(hot0 * count, axis=0, keepdims=True).astype(jnp.int32)
    rank1 = jnp.sum(hot1 * count, axis=0, keepdims=True).astype(jnp.int32)
    slot0 = picks[0:1, :] * 16 + rank0
    slot1 = picks[1:2, :] * 16 + rank1
    slot_out[0:1, :] = slot0
    slot_out[1:2, :] = slot1
    slot = lax.broadcasted_iota(jnp.int32, (512, 128), 0)
    placing = jnp.where((slot == slot0) | (slot == slot1), 1.0, 0.0).astype(BF16)
    out[...] = contract(placing, u, ((1,), (0,))).astype(BF16)


def expert_body(
    place, rows, gain, shift, gate0, up0, down0, gate1, up1, down1, out, normed
):
    total = rows[0].astype(F32)
    for n in range(1, 16):
        total = total + rows[n].astype(F32)
    mean = jnp.sum(total, axis=-1, keepdims=True) * (1.0 / 2048)
    square = jnp.zeros(total.shape, F32)
    for n in range(16):
        centred = rows[n].astype(F32) - mean
        square = square + centred * centred
    rstd = lax.rsqrt(jnp.sum(square, axis=-1, keepdims=True) * (1.0 / 2048) + NORM_EPS)
    for n in range(16):
        cols = slice(n * 128, (n + 1) * 128)
        piece = (rows[n].astype(F32) - mean) * rstd * gain[:, cols] + shift[:, cols]
        piece = piece.astype(BF16).reshape(16, 2, 16, 128)
        normed[0, :, cols] = piece[:, 0].reshape(256, 128)
        normed[1, :, cols] = piece[:, 1].reshape(256, 128)
    c = place[1]
    for which, gate_w, up_w, down_w in ((c, gate0, up0, down0), (1 - c, gate1, up1, down1)):
        piece = normed[which]
        gate = contract(piece, gate_w[...], ((1,), (0,)))
        upper = contract(piece, up_w[...], ((1,), (0,)))
        hidden = (gate / (1.0 + jnp.exp(-gate)) * upper).astype(BF16)
        for n in range(8):
            term = contract(hidden, down_w[:, n * 256 : (n + 1) * 256], ((1,), (0,)))
            term = term.astype(BF16)
            out[2 * n, :, which] = term[:, 0:128].reshape(16, 16, 128)
            out[2 * n + 1, :, which] = term[:, 128:256].reshape(16, 16, 128)


def sum_body(arrived, out):
    total = arrived[0].astype(F32)
    for n in range(1, 16):
        total = total + arrived[n].astype(F32)
    out[...] = total.astype(BF16)


def mix_body(returned, slots, weight, u, out):
    slot = lax.broadcasted_iota(jnp.int32, (512, 128), 0)
    total = jnp.zeros((128, 128), F32)
    for k in range(2):
        placing = jnp.where(slot == slots[k : k + 1, :], 1.0, 0.0).astype(BF16)
        picked = contract(placing, returned[...], ((0,), (0,)))
        total = total + weight[:, k : k + 1] * picked
    out[:, :, 0:128] = u[...].reshape(16, 8, 128)
    out[:, :, 128:256] = total.astype(BF16).reshape(16, 8, 128)


def layer_norm(inputs, gain_vec, shift_vec):
    average = jnp.mean(inputs, axis=-1, keepdims=True)
    centred = inputs - average
    variance = jnp.mean(centred * centred, axis=-1, keepdims=True)
    return centred * lax.rsqrt(variance + NORM_EPS) * gain_vec + shift_vec


def final_body(arrived, gain1, shift1, gain2, shift2, out):
    u = jnp.concatenate([arrived[n, :, 0:128] for n in range(16)], axis=1).astype(F32)
    mix = jnp.concatenate([arrived[n, :, 128:256] for n in range(16)], axis=1).astype(F32)
    normed = layer_norm(u, gain1[...], shift1[...]).astype(BF16).astype(F32)
    out[...] = layer_norm(ALPHA_RES * normed + mix, gain2[...], shift2[...]).astype(BF16)


def shape(dims, dtype=BF16):
    return jax.ShapeDtypeStruct(dims, dtype)


def with_place(body, place, out_shape, *args, scratch=(), blocks=None):
    def whole(dims):
        return pl.BlockSpec(dims, lambda i, p, n=len(dims): (0,) * n)

    specs = [whole(arg.shape) for arg in args]
    for at, spec in (blocks or {}).items():
        specs[at] = spec
    outs = out_shape if isinstance(out_shape, list) else [out_shape]
    out_specs = [whole(o.shape) for o in outs]
    return pl.pallas_call(
        body,
        grid_spec=pltpu.PrefetchScalarGridSpec(
            num_scalar_prefetch=1,
            grid=(1,),
            in_specs=specs,
            out_specs=out_specs if isinstance(out_shape, list) else out_specs[0],
            scratch_shapes=list(scratch),
        ),
        out_shape=out_shape,
        compiler_params=pltpu.CompilerParams(vmem_limit_bytes=48 * 1024 * 1024),
    )(place, *args)


SWAP = ((0, 1), (1, 0))


def local(
    stream,
    query_small,
    key_small,
    value_small,
    query_large,
    key_large,
    value_large,
    key_bias,
    out_small,
    out_large,
    gain_one,
    shift_one,
    gain_two,
    shift_two,
    expert_pick,
    route_weight,
    w_gate,
    w_up,
    w_down,
):
    place = jnp.stack(
        [lax.axis_index(name) for name in ("a", "c", "b")] + [lax.axis_index(TP)]
    ).astype(jnp.int32)
    bias = key_bias.reshape(128, 2).T.reshape(1, 256)
    bias = jnp.broadcast_to(jnp.pad(bias, ((0, 0), (0, 128))), (16, 384))
    kv, q = call(
        pack_body,
        [shape((4, 144, 384)), shape((128, 256))],
        key_small, value_small, key_large, value_large, query_small, query_large, bias,
    )
    weights = (w_gate[0], w_up[0], w_down[0])
    q_far = [lax.ppermute(q, "a", [(i + d, i) for i in range(4 - d)]) for d in (1, 2, 3)]
    own = lax.all_to_all(kv, "b", 0, 0, tiled=True)
    other = lax.ppermute(own, "c", SWAP)
    keys = [pltpu.VMEM((1024, 384), BF16), pltpu.VMEM((8, 1024), F32)]
    far = with_place(
        far_body, place, [shape((128, 256))] * 3, *q_far, own, other,
        scratch=keys + [pltpu.VMEM((384, 256), BF16)],
    )
    back = [
        lax.ppermute(far[d - 1], "a", [(i, i + d) for i in range(4 - d)]) for d in (1, 2, 3)
    ]
    near = with_place(near_body, place, shape((128, 256), F32), q, own, other, scratch=keys)
    partial = call(project_body, shape((16, 128, 128)), near, *back, out_small, out_large)
    arrived = lax.all_to_all(partial, TP, 0, 0, tiled=True)
    u, slots, outgoing = with_place(
        route_body, place,
        [shape((128, 128)), shape((8, 128), jnp.int32), shape((512, 128))],
        arrived, stream, expert_pick.T,
        blocks={1: pl.BlockSpec((128, 128), lambda i, p: (0, p[3]))},
    )
    moved = lax.all_to_all(outgoing.reshape(16, 32, 128), ("a", "b"), 0, 0, tiled=True)
    rows = lax.all_to_all(
        jnp.broadcast_to(moved.reshape(1, 512, 128), (16, 512, 128)), TP, 0, 0, tiled=True
    )
    partner = [lax.ppermute(w, "c", SWAP) for w in weights]
    terms = with_place(
        expert_body, place, shape((16, 16, 2, 16, 128)),
        rows, gain_one.reshape(1, 2048), shift_one.reshape(1, 2048), *weights, *partner,
        scratch=[pltpu.VMEM((2, 256, 2048), BF16)],
    )
    summed = call(
        sum_body, shape((512, 128)),
        lax.all_to_all(terms.reshape(16, 512, 128), TP, 0, 0, tiled=True),
    )
    returned = lax.all_to_all(summed.reshape(16, 32, 128), ("a", "b"), 0, 0, tiled=True)
    mixed = call(
        mix_body, shape((16, 8, 256)), returned.reshape(512, 128), slots, route_weight, u
    )
    last = lax.all_to_all(mixed, TP, 0, 0, tiled=True)
    vectors = [v.reshape(1, 2048) for v in (gain_one, shift_one, gain_two, shift_two)]
    return call(final_body, shape((8, 2048)), last, *vectors)


def solution(mesh):
    torus = Mesh(mesh.devices.reshape(4, 4, 2, 4, 4), ("a", "b", "c", "y", "x"))
    in_specs = (
        P(SP, None),
        P(SP, TP),
        P(SP, TP),
        P(SP, TP),
        P(SP, TP),
        P(SP, TP),
        P(SP, TP),
        P(SP, None, TP),
        P(TP, None),
        P(TP, None),
        P(),
        P(),
        P(),
        P(),
        P(SP, None),
        P(SP, None),
        P(SP, None, TP),
        P(SP, None, TP),
        P(SP, TP, None),
    )
    out_specs = P(SP + TP, None)
    return jax.shard_map(local, mesh=torus, in_specs=in_specs, out_specs=out_specs, check_vma=False)
```
